32 devices in a mesh: fs: 8 (over z, x), tp: 4 (over y, core).
Axes of the slice: x: 2, y: 2, z: 4, core: 2. Of those that a mesh axis runs over, the one named last changes fastest.
Arguments:
- inputs: bfloat16 [8192, 2048], P('fs'), may hold values from -6 to 6
- cotangents: bfloat16 [8192, 3, 1024], P('fs', None, 'tp'), may hold values from -0.06591797 to 0.06591797
- factors: bfloat16 [3, 2048, 256], P(None, 'fs'), may hold values from -13.810679 to 13.810679
- first_moment: float32 [3, 256, 1024], P(None, None, 'tp'), may hold values from -6 to 6
- second_moment: float32 [3, 256, 1024], P(None, None, 'tp'), may hold values from 0.05 to 1
- master: float32 [3, 2048, 1024], P(None, 'fs', 'tp'), may hold values from -0.125 to 0.125
Outputs:
- update_step: float32 [3, 2048, 1024], P(None, 'fs', 'tp')
- new_master: float32 [3, 2048, 1024], P(None, 'fs', 'tp')
- new_copy: bfloat16 [3, 2048, 1024], P(None, None, 'tp')
- new_first: float32 [3, 256, 1024], P(None, None, 'tp')
- new_second: float32 [3, 256, 1024], P(None, None, 'tp')
The draws below stay inside these ranges and needn't reach their ends.
All inputs are finite; a program needn't handle non-finite values.
Results may differ from the reference program's by a relative error of at most 0.001.
Values may be sent and summed in bfloat16 or wider, within the bound.
No kernel may reach another device: no remote copies, remote signals or barrier semaphores. Data moves between devices by JAX's collectives and lax.ppermute only.
A program may use at most 64 MiB of HBM per device.

```python
import math
import jax
import jax.numpy as jnp
from jax import lax

D = 2048
MW = 1024
RANK = 256
MATS = 3
TOKENS = 8192


def draw_factors(key, part):
    keys = jax.random.split(jax.random.fold_in(key, 17), 3)
    position = jnp.arange(D, dtype=jnp.float32) / (D - 1)
    base = jnp.clip(jax.random.normal(keys[0], (MATS, D, RANK), jnp.float32), -5.0, 5.0)
    ramp = jnp.exp(math.log(5.0) * position)
    row_scale = jnp.exp(jax.random.uniform(keys[1], (MATS, D, 1), jnp.float32, 0.0, math.log(10.0)))
    col_scale = jnp.exp(jax.random.uniform(keys[2], (MATS, 1, RANK), jnp.float32, 0.0, math.log(10.0)))
    value = base * ramp[None, :, None] * row_scale * col_scale / (8.0 * math.sqrt(D))
    return value.astype(jnp.bfloat16)


def strengthened(values, stream_key, source, target, parts, factor):
    def block_of(axis_at):
        return (jnp.arange(values.shape[axis_at]) // (values.shape[axis_at] // parts)).reshape((-1,) + (1,) * (values.ndim - 1 - axis_at))

    one_side = jax.random.permutation(stream_key, parts)[block_of(target)]
    far = (block_of(target) + parts // 2) % parts
    return jnp.where((block_of(source) == one_side) | (block_of(source) == far), factor * values, values)


def block_levels(key, dims, pieces, least, high):
    factor_of = 1.0
    for dim, parts in pieces:
        heights = jax.random.uniform(jax.random.fold_in(jax.random.fold_in(key, 6), dim), (parts,), jnp.float32, least / len(pieces), high / len(pieces))
        factor_of = factor_of * jnp.repeat(jnp.exp(heights), dims[dim] // parts).reshape((-1,) + (1,) * (len(dims) - 1 - dim))
    return factor_of


def normal_values(rng, shape, deviation, bound, cuts=(), held_as=jnp.bfloat16):
    values = deviation * jax.random.normal(rng, shape, jnp.float32)
    if cuts:
        values = values * block_levels(rng, shape, cuts, -0.22, 0.18)
    return jnp.clip(values, -bound, bound).astype(held_as)


def noise_with(rng, shape, spread, limit, cuts, heavy, kind=jnp.bfloat16):
    entries = spread * jax.random.normal(rng, shape, jnp.float32)
    if cuts:
        entries = entries * block_levels(rng, shape, cuts, -0.22, 0.18)
    return jnp.clip(strengthened(entries, jax.random.fold_in(rng, 3), *heavy), -limit, limit).astype(kind)


def setup_inputs(seed: int = 0) -> dict:
    streams_of = jax.random.split(jax.random.key(seed), 7)
    inputs = noise_with(streams_of[0], (TOKENS, D), 1.0, 6.0, ((0, 8),), (0, 1, 8, 2.0))
    cotangents = normal_values(streams_of[1], (TOKENS, MATS, MW), (1.0 / TOKENS ** 0.5), 0.06591797, ((0, 8), (2, 4)))
    factors = draw_factors(jax.random.fold_in(streams_of[6], 71), 0)
    first_moment = normal_values(streams_of[3], (MATS, RANK, MW), 1.0, 6.0, ((2, 4),), jnp.float32)
    second_moment = jnp.clip(jnp.exp(math.log(1.0) - 2.9957323 * jax.random.uniform(streams_of[4], (MATS, RANK, MW), jnp.float32) ** block_levels(streams_of[4], (MATS, RANK, MW), ((2, 4),), -0.2, 0.2)), 0.05, 1.0)
    master = normal_values(streams_of[5], (MATS, D, MW), D ** -0.5, 0.125, ((1, 8), (2, 4)), jnp.float32)
    return {"inputs": inputs, "cotangents": cotangents, "factors": factors, "first_moment": first_moment, "second_moment": second_moment, "master": master}


beta_first = 0.8
beta_second = 0.9
adam_eps = 1e-08
norm_eps = 1e-06
learning_rate = 0.005

def reference(inputs, cotangents, factors, first_moment, second_moment, master):
    flat_cot = cotangents.reshape(cotangents.shape[0], MATS * MW)
    gradient = lax.dot_general(inputs, flat_cot, (((0,), (0,)), ((), ())), preferred_element_type=jnp.float32)
    gradient = gradient.reshape(D, MATS, MW).transpose(1, 0, 2)
    factor32 = factors.astype(jnp.float32)
    projected = jnp.einsum('mdr,mdc->mrc', factor32, gradient, precision=lax.Precision.HIGHEST)
    new_first = beta_first * first_moment + (1.0 - beta_first) * projected
    new_second = beta_second * second_moment + (1.0 - beta_second) * projected * projected
    normed = new_first / (jnp.sqrt(new_second) + adam_eps)
    update = jnp.einsum('mdr,mrc->mdc', factor32, normed, precision=lax.Precision.HIGHEST)
    root_mean = jnp.sqrt(lax.optimization_barrier(jnp.mean(update * update, axis=(1, 2))) + norm_eps)
    update_step = update / root_mean[:, None, None]
    new_master = master - learning_rate * update_step
    new_copy = new_master.astype(jnp.bfloat16)
    return (update_step, new_master, new_copy, new_first, new_second)
```

```python
import jax
import jax.numpy as jnp
from jax import lax
from jax.sharding import Mesh, PartitionSpec as P

beta_first = 0.8
beta_second = 0.9
adam_eps = 1e-08
norm_eps = 1e-06
learning_rate = 0.005

FS = ("z", "x")
PAIR = 2
LONGEST_LINE = 4


def split_two(value):
    high = lax.reduce_precision(value, 8, 7)
    return high.astype(jnp.bfloat16), (value - high).astype(jnp.bfloat16)


def line_shift(value, distance, step, nz):
    pairs = []
    for z in range(nz):
        if 0 <= z - step * (distance - 1) < nz and 0 <= z + step < nz:
            pairs += [(z * PAIR + x, (z + step) * PAIR + x) for x in range(PAIR)]
    return lax.ppermute(value, FS, pairs)


def swap_x(value, distance, step, nz):
    pairs = []
    for z in range(nz):
        if 0 <= z - step * distance < nz:
            pairs += [(z * PAIR + x, z * PAIR + 1 - x) for x in range(PAIR)]
    return lax.ppermute(value, FS, pairs)


def gather_fs(value, nz):
    mats, rows, cols = value.shape
    if nz > LONGEST_LINE:
        return lax.all_gather(value, FS, axis=1, tiled=True)
    up, down = {0: value}, {0: value}
    up_x = {0: swap_x(value, 0, 1, nz)}
    down_x = {0: up_x[0]}
    for k in range(1, nz):
        up[k] = line_shift(up[k - 1], k, 1, nz)
        down[k] = line_shift(down[k - 1], k, -1, nz)
        up_x[k] = swap_x(up[k], k, 1, nz)
        down_x[k] = swap_x(down[k], k, -1, nz)
    z, x = lax.axis_index("z"), lax.axis_index("x")
    out = jnp.zeros((mats, nz * PAIR, rows, cols), value.dtype)
    for k in range(nz):
        source = (z - k) % nz
        if k:
            mine = jnp.where(z >= k, up[k], down[nz - k])
            theirs = jnp.where(z >= k, up_x[k], down_x[nz - k])
        else:
            mine, theirs = value, up_x[0]
        out = lax.dynamic_update_slice(out, mine[:, None], (0, source * PAIR + x, 0, 0))
        out = lax.dynamic_update_slice(out, theirs[:, None], (0, source * PAIR + 1 - x, 0, 0))
    return out.reshape(mats, nz * PAIR * rows, cols)


def solution(mesh):
    nfs, ntp = mesh.shape["fs"], mesh.shape["tp"]
    nz = nfs // PAIR
    grid = Mesh(mesh.devices.reshape(nz, PAIR, ntp // PAIR, PAIR), ("z", "x", "y", "core"))
    swap = [(0, 1), (1, 0)]

    def local(inputs, cotangents, factors, first_moment, second_moment, master):
        mats, rows, rank = factors.shape
        cols = cotangents.shape[2]
        half = rank // PAIR
        core = lax.axis_index("core")
        my_half = lax.dynamic_slice_in_dim(factors, core * half, half, 2)
        cot_other = lax.ppermute(cotangents, "core", swap)
        wide = gather_fs(my_half, nz)
        wide_other = lax.ppermute(wide, "core", swap)
        lowered = jnp.einsum("tk,mkr->mtr", inputs, wide, preferred_element_type=jnp.float32)
        pair = jnp.concatenate(split_two(lowered), axis=2)

        def contract(cot):
            both = jnp.einsum("mtr,tmc->mrc", pair, cot, preferred_element_type=jnp.float32)
            return both[:, :half] + both[:, half:]

        partial = jnp.stack([contract(cotangents), contract(cot_other)])
        chunk = half // nfs
        partial = partial.reshape(PAIR, mats, nfs, chunk, cols).transpose(2, 0, 1, 3, 4)
        reduced = jnp.sum(lax.all_to_all(partial, FS, 0, 0), axis=0)
        ordered = jnp.where(core == 0, reduced, reduced[::-1])
        sent = jnp.broadcast_to(ordered[None], (nfs,) + ordered.shape).reshape((nfs * PAIR,) + ordered.shape[1:])
        got = lax.all_to_all(sent, ("z", "x", "core"), 0, 0)
        got = got.reshape(nfs, PAIR, mats, chunk, cols).transpose(2, 1, 0, 3, 4)
        projected = got.reshape(mats, rank, cols)

        new_first = beta_first * first_moment + (1.0 - beta_first) * projected
        new_second = beta_second * second_moment + (1.0 - beta_second) * projected * projected
        normed = new_first / (jnp.sqrt(new_second) + adam_eps)
        terms = jnp.concatenate(split_two(normed), axis=2)

        def expand(factor, rhs):
            both = jnp.einsum("mdr,mrc->mdc", factor, rhs, preferred_element_type=jnp.float32)
            return both[:, :, :cols] + both[:, :, cols:]

        update = expand(factors, terms)
        turned = jnp.where(core == 0, terms, jnp.roll(terms, half, axis=1))
        whole = expand(jnp.concatenate([wide, wide_other], axis=2), turned)
        squares = lax.psum(jnp.sum(whole * whole, axis=(1, 2)), ("y", "core"))
        size = (nfs * rows) * (ntp * cols)
        root_mean = jnp.sqrt(squares / size + norm_eps)
        update_step = update / root_mean[:, None, None]
        new_master = master - learning_rate * update_step
        new_copy = gather_fs(new_master.astype(jnp.bfloat16), nz)
        return (update_step, new_master, new_copy, new_first, new_second)

    tp = ("y", "core")
    placed = (
        P(FS, None),
        P(FS, None, tp),
        P(None, FS, None),
        P(None, None, tp),
        P(None, None, tp),
        P(None, FS, tp),
    )
    return jax.shard_map(
        local,
        mesh=grid,
        in_specs=placed,
        out_specs=(
            P(None, FS, tp),
            P(None, FS, tp),
            P(None, None, tp),
            P(None, None, tp),
            P(None, None, tp),
        ),
        check_vma=False,
    )
```

```python
import jax
import jax.numpy as jnp
from jax import lax
from jax.sharding import Mesh, PartitionSpec as P


beta_first = 0.8
beta_second = 0.9
adam_eps = 1e-08
norm_eps = 1e-06
learning_rate = 0.005

FS = ("z", "x")
PAIR = 2
LONGEST_LINE = 4


def split_two(value):
    high = lax.reduce_precision(value, 8, 7)
    return high.astype(jnp.bfloat16), (value - high).astype(jnp.bfloat16)


def pack_half(value):
    n, _, mats, _, cols = value.shape
    most = jnp.max(jnp.abs(value), axis=(0, 1, 3, 4))
    exponent = jnp.ceil(jnp.log2(jnp.maximum(most, 1e-30))) - 14.0
    scaled = (value * jnp.exp2(-exponent)[None, None, :, None, None]).astype(jnp.float16)
    row = jnp.pad(exponent, (0, cols - mats)).astype(jnp.float16)
    row = jnp.broadcast_to(row[None, None], (n, 1, cols))
    return jnp.concatenate([scaled.reshape(n, -1, cols), row], axis=1)


def unpack_half(packed, shape):
    _, _, mats, _, _ = shape
    values = packed[:, :-1].astype(jnp.float32).reshape(shape)
    scale = jnp.exp2(packed[:, -1, :mats].astype(jnp.float32))
    return values * scale[:, None, :, None, None]


def line_shift(value, distance, step, nz):
    pairs = []
    for z in range(nz):
        if 0 <= z - step * (distance - 1) < nz and 0 <= z + step < nz:
            pairs += [(z * PAIR + x, (z + step) * PAIR + x) for x in range(PAIR)]
    return lax.ppermute(value, FS, pairs)


def swap_x(value, distance, step, nz):
    pairs = []
    for z in range(nz):
        if 0 <= z - step * distance < nz:
            pairs += [(z * PAIR + x, z * PAIR + 1 - x) for x in range(PAIR)]
    return lax.ppermute(value, FS, pairs)


def gather_fs(value, nz):
    mats, rows, cols = value.shape
    if nz > LONGEST_LINE:
        return lax.all_gather(value, FS, axis=1, tiled=True)
    up, down = {0: value}, {0: value}
    up_x = {0: swap_x(value, 0, 1, nz)}
    down_x = {0: up_x[0]}
    for k in range(1, nz):
        up[k] = line_shift(up[k - 1], k, 1, nz)
        down[k] = line_shift(down[k - 1], k, -1, nz)
        up_x[k] = swap_x(up[k], k, 1, nz)
        down_x[k] = swap_x(down[k], k, -1, nz)
    z, x = lax.axis_index("z"), lax.axis_index("x")
    out = jnp.zeros((mats, nz * PAIR, rows, cols), value.dtype)
    for k in range(nz):
        source = (z - k) % nz
        if k:
            mine = jnp.where(z >= k, up[k], down[nz - k])
            theirs = jnp.where(z >= k, up_x[k], down_x[nz - k])
        else:
            mine, theirs = value, up_x[0]
        out = lax.dynamic_update_slice(out, mine[:, None], (0, source * PAIR + x, 0, 0))
        out = lax.dynamic_update_slice(out, theirs[:, None], (0, source * PAIR + 1 - x, 0, 0))
    return out.reshape(mats, nz * PAIR * rows, cols)


def solution(mesh):
    nfs, ntp = mesh.shape["fs"], mesh.shape["tp"]
    nz = nfs // PAIR
    grid = Mesh(mesh.devices.reshape(nz, PAIR, ntp // PAIR, PAIR), ("z", "x", "y", "core"))
    swap = [(0, 1), (1, 0)]

    def step(inputs, cotangents, factors, first_moment, second_moment, master):
        mats, rows, rank = factors.shape
        cols = cotangents.shape[2]
        half = rank // PAIR
        core = lax.axis_index("core")
        my_half = lax.dynamic_slice_in_dim(factors, core * half, half, 2)
        cot_other = lax.ppermute(cotangents, "core", swap)
        wide = gather_fs(my_half, nz)
        wide_other = lax.ppermute(wide, "core", swap)
        lowered = jnp.einsum("tk,mkr->mtr", inputs, wide, preferred_element_type=jnp.float32)
        pair = jnp.concatenate(split_two(lowered), axis=2)

        def contract(cot):
            both = jnp.einsum("mtr,tmc->mrc", pair, cot, preferred_element_type=jnp.float32)
            return both[:, :half] + both[:, half:]

        partial = jnp.stack([contract(cotangents), contract(cot_other)])
        chunk = half // nfs
        partial = partial.reshape(PAIR, mats, nfs, chunk, cols).transpose(2, 0, 1, 3, 4)
        arrived = lax.all_to_all(pack_half(partial), FS, 0, 0)
        reduced = jnp.sum(unpack_half(arrived, partial.shape), axis=0)
        ordered = jnp.where(core == 0, reduced, reduced[::-1])
        packed = pack_half(ordered[:, None])
        sent = jnp.broadcast_to(packed[None], (nfs,) + packed.shape).reshape((nfs * PAIR,) + packed.shape[1:])
        got = lax.all_to_all(sent, ("z", "x", "core"), 0, 0)
        got = unpack_half(got, (nfs * PAIR, 1) + ordered.shape[1:])
        got = got.reshape(nfs, PAIR, mats, chunk, cols).transpose(2, 1, 0, 3, 4)
        projected = got.reshape(mats, rank, cols)

        new_first = beta_first * first_moment + (1.0 - beta_first) * projected
        new_second = beta_second * second_moment + (1.0 - beta_second) * projected * projected
        normed = new_first / (jnp.sqrt(new_second) + adam_eps)
        terms = jnp.concatenate(split_two(normed), axis=2)

        def expand(factor, rhs):
            both = jnp.einsum("mdr,mrc->mdc", factor, rhs, preferred_element_type=jnp.float32)
            return both[:, :, :cols] + both[:, :, cols:]

        update = expand(factors, terms)
        turned = jnp.where(core == 0, terms, jnp.roll(terms, half, axis=1))
        whole = expand(jnp.concatenate([wide, wide_other], axis=2), turned)
        squares = lax.psum(jnp.sum(whole * whole, axis=(1, 2)), ("y", "core"))
        size = (nfs * rows) * (ntp * cols)
        root_mean = jnp.sqrt(squares / size + norm_eps)
        update_step = update / root_mean[:, None, None]
        new_master = master - learning_rate * update_step
        new_copy = gather_fs(new_master.astype(jnp.bfloat16), nz)
        return (update_step, new_master, new_copy, new_first, new_second)

    tp = ("y", "core")
    placed = (
        P(FS, None),
        P(FS, None, tp),
        P(None, FS, None),
        P(None, None, tp),
        P(None, None, tp),
        P(None, FS, tp),
    )
    return jax.shard_map(
        step,
        mesh=grid,
        in_specs=placed,
        out_specs=(
            P(None, FS, tp),
            P(None, FS, tp),
            P(None, None, tp),
            P(None, None, tp),
            P(None, None, tp),
        ),
        check_vma=False,
    )
```
